32 devices in a mesh: rep: 2 (over y), fs: 4 (over z), tp: 4 (over x, core).
Axes of the slice: x: 2, y: 2, z: 4, core: 2. Of those that a mesh axis runs over, the one named last changes fastest.
Arguments:
- stream: bfloat16 [4096, 2048], P(('rep', 'fs'), 'tp'), parts along dimension 0, may hold values from -6 to 6
- in_weight: bfloat16 [2048, 1024], P('fs', 'tp'), may hold values from -0.125 to 0.125
- pool_weight: bfloat16 [8, 128, 128], P('tp'), may hold values from -0.5 to 0.5
- pool_scale: bfloat16 [1024], P('tp'), may hold values from 0.099609375 to 1.8984375
- out_weight: bfloat16 [1024, 2048], P('tp', 'fs'), may hold values from -0.1875 to 0.1875
- mix_gain: bfloat16 [2048], replicated, may hold values from 0.099609375 to 1.8984375
- ffn_gain: bfloat16 [2048], replicated, may hold values from 0.099609375 to 1.8984375
- gate_weight: bfloat16 [2048, 5632], P('fs', 'tp'), may hold values from -0.125 to 0.125
- up_weight: bfloat16 [2048, 5632], P('fs', 'tp'), may hold values from -0.125 to 0.125
- down_weight: bfloat16 [5632, 2048], P('tp', 'fs'), may hold values from -0.078125 to 0.078125
Outputs:
- result: bfloat16 [4096, 2048], P(('rep', 'fs'), 'tp'), parts along dimension 0
The draws below stay inside these ranges and needn't reach their ends.
There are 2 independent parts, one for each index of `rep`. The reference program is written for one: setup_inputs(seed, part) draws one part's arguments, and reference() takes and returns one part's arrays. A program takes and returns all parts, laid end to end along the dimension named above; an argument that names none is the same for every part. Nothing has to cross between parts.
All inputs are finite; a program needn't handle non-finite values.
Results may differ from the reference program's by a relative error of at most 0.015.
Values may be sent and summed in bfloat16 or wider, within the bound.
A program may use at most 64 MiB of HBM per device.

```python
import jax
import jax.numpy as jnp
from jax import lax

D = 2048
GROUPS = 8
GROUP_DIM = 128
FF = 5632
SEQ = 128
POOL_CH = 1024
TOKENS = 2048
N_TP = 4


def block_scale(own_key, shape, split, least, high):
    factor_of, own = 1.0, jax.random.fold_in(own_key, 6)
    for axis_at, parts in split:
        steps = jnp.exp(jax.random.uniform(jax.random.fold_in(own, axis_at), (parts,), jnp.float32, least / len(split), high / len(split)))
        factor_of = factor_of * jnp.repeat(steps, shape[axis_at] // parts).reshape([-1 if axis == axis_at else 1 for axis in range(len(shape))])
    return factor_of


def bell_draw(rng, extent, width, bound, cuts=(), kind=jnp.bfloat16):
    array = width * jax.random.normal(rng, extent, jnp.float32)
    if cuts:
        array = array * block_scale(rng, extent, cuts, -0.22, 0.18)
    return jnp.clip(array, -bound, bound).astype(kind)


def setup_inputs(seed: int = 0, part: int = 0) -> dict:
    keys = jax.random.split(jax.random.key(seed), 11)
    part_keys = jax.random.split(jax.random.fold_in(keys[10], part), 11)
    return {
        "stream": bell_draw(part_keys[0], (TOKENS, D), 1.0, 6.0, ((0, 4), (1, 4))),
        "in_weight": bell_draw(keys[1], (D, POOL_CH), D ** -0.5, 0.125, ((0, 4), (1, 4))),
        "pool_weight": bell_draw(keys[2], (GROUPS, GROUP_DIM, GROUP_DIM), GROUP_DIM ** -0.5, 0.5, ((0, 4),)),
        "pool_scale": jnp.clip(1.0 + 0.18 * jax.random.normal(keys[3], (POOL_CH,), jnp.float32), 0.099609375, 1.8984375).astype(jnp.bfloat16),
        "out_weight": bell_draw(keys[4], (POOL_CH, D), POOL_CH ** -0.5, 0.1875, ((0, 4), (1, 4))),
        "mix_gain": jnp.clip(1.0 + 0.18 * jax.random.normal(keys[5], (D,), jnp.float32), 0.099609375, 1.8984375).astype(jnp.bfloat16),
        "ffn_gain": jnp.clip(1.0 + 0.18 * jax.random.normal(keys[6], (D,), jnp.float32), 0.099609375, 1.8984375).astype(jnp.bfloat16),
        "gate_weight": bell_draw(keys[7], (D, FF), D ** -0.5, 0.125, ((0, 4), (1, 4))),
        "up_weight": bell_draw(keys[8], (D, FF), D ** -0.5, 0.125, ((0, 4), (1, 4))),
        "down_weight": bell_draw(keys[9], (FF, D), FF ** -0.5, 0.078125, ((0, 4), (1, 4))),
    }


epsilon = 1e-06

def root_norm(values, gain_vec):
    widened = values.astype(jnp.float32)
    scaled = widened * lax.rsqrt(lax.optimization_barrier(jnp.mean(widened * widened, axis=-1, keepdims=True)) + epsilon)
    return (scaled * gain_vec.astype(jnp.float32)).astype(jnp.bfloat16)

def window_tables(first_group, group_count, seq_len, total_groups):
    group_ids = first_group + jnp.arange(group_count, dtype=jnp.int32)
    reaches = jnp.left_shift(jnp.int32(2), 4 * group_ids // total_groups)
    query_pos = jnp.arange(seq_len, dtype=jnp.int32)[:, None]
    earlier = jnp.arange(seq_len, dtype=jnp.int32)[None, :]
    inside = (earlier <= query_pos)[None] & (earlier[None] > query_pos[None] - reaches[:, None, None])
    counts = jnp.minimum(query_pos[:, 0][None, :] + 1, reaches[:, None]).astype(jnp.float32)
    return (inside, counts)

def block_sum(operand, weights):
    block_width = operand.shape[1] // N_TP
    running = jnp.zeros((operand.shape[0], weights.shape[1]), jnp.float32)
    for block_id in range(N_TP):
        product = jnp.dot(operand[:, block_id * block_width:(block_id + 1) * block_width], weights[block_id * block_width:(block_id + 1) * block_width], preferred_element_type=jnp.float32)
        rounded = lax.optimization_barrier(product.astype(jnp.bfloat16))
        running = running + rounded.astype(jnp.float32)
    return running

def reference(stream, in_weight, pool_weight, pool_scale, out_weight, mix_gain, ffn_gain, gate_weight, up_weight, down_weight):
    normed = root_norm(stream, mix_gain)
    pooled_in = jnp.dot(normed, in_weight, preferred_element_type=jnp.float32).astype(jnp.bfloat16)
    inside, counts = window_tables(0, GROUPS, SEQ, GROUPS)
    grouped = pooled_in.astype(jnp.float32).reshape(TOKENS // SEQ, SEQ, GROUPS, GROUP_DIM)
    window_sums = jnp.einsum('gts,nsgc->ntgc', inside.astype(jnp.float32), grouped, precision=lax.Precision.HIGHEST)
    contrast = (window_sums / counts.T[None, :, :, None] - grouped).astype(jnp.bfloat16)
    mixed_out = jnp.einsum('ntgc,gcd->ntgd', contrast.astype(jnp.float32), pool_weight.astype(jnp.float32))
    group_out = (mixed_out.reshape(TOKENS, POOL_CH) * pool_scale.astype(jnp.float32)).astype(jnp.bfloat16)
    mixer_sum = block_sum(group_out, out_weight)
    middle = (stream.astype(jnp.float32) + mixer_sum).astype(jnp.bfloat16)
    normed_ffn = root_norm(middle, ffn_gain)
    gate_acts = jnp.dot(normed_ffn, gate_weight, preferred_element_type=jnp.float32)
    up_acts = jnp.dot(normed_ffn, up_weight, preferred_element_type=jnp.float32)
    hidden = (jax.nn.silu(gate_acts) * up_acts).astype(jnp.bfloat16)
    ffn_sum = block_sum(hidden, down_weight)
    return (middle.astype(jnp.float32) + ffn_sum).astype(jnp.bfloat16)
```

```python
import functools

import jax
import jax.numpy as jnp
from jax import lax
from jax.experimental import pallas as pl
from jax.experimental.pallas import tpu as pltpu
from jax.sharding import PartitionSpec as P

SEQ = 128
EPSILON = 1e-06
MESH = pl.DeviceIdType.MESH
KINDS = (("in", True, False), ("out", False, False), ("up", True, True),
         ("down", False, True), ("gate", True, False))


def kernel(sizes, stream, in_w, out_w, up_w, down_w, gate_w, pool_w, scale,
           mix_gain, ffn_gain, result,
           in_all, out_all, up_all, down_all, gate_all,
           rows_all, normed, group_out, hidden, middle, mid_all,
           mix_send, mix_recv, ffn_send, ffn_recv,
           ring_send, ring_recv, fwd_send, fwd_recv, own_sem,
           tp_send, tp_recv, keep_sem):
    reps, fs, tp = sizes
    half = fs // 2
    my_rep, me, my_tp = lax.axis_index("rep"), lax.axis_index("fs"), lax.axis_index("tp")
    own = (in_w, out_w, up_w, down_w, gate_w)
    full = (in_all, out_all, up_all, down_all, gate_all)
    tokens, width = stream.shape

    def turn(at, by, count):
        return lax.rem(at + by + count, count)

    def piece(which, owner, row, count):
        block_rows, block_cols = own[which].shape
        if KINDS[which][1]:
            return full[which].at[pl.ds(pl.multiple_of(owner * block_rows + row, 16), count), :]
        return full[which].at[pl.ds(pl.multiple_of(row, 16), count),
                              pl.ds(pl.multiple_of(owner * block_cols, 128), block_cols)]

    def span(which, step, way):
        count = own[which].shape[0]
        row = 0
        if KINDS[which][2]:
            count = count // reps
            row = my_rep * count
        if step == half:
            count = count // 2
            row = row + way * count
        return row, count

    def ring(which, step, way):
        row, count = span(which, step, way)
        sign = 1 - 2 * way
        owner = turn(me, -sign * (step - 1), fs)
        if step == 1:
            source = own[which].at[pl.ds(pl.multiple_of(row, 16), count), :]
        else:
            source = piece(which, owner, row, count)
        return pltpu.make_async_remote_copy(
            src_ref=source, dst_ref=piece(which, owner, row, count),
            send_sem=ring_send.at[which, step - 1, way],
            recv_sem=ring_recv.at[which, step - 1, way],
            device_id={"fs": turn(me, sign, fs)}, device_id_type=MESH)

    def forward(which, step, way, peer):
        row, count = span(which, step, way)
        owner = turn(me, -(1 - 2 * way) * step, fs)
        block = piece(which, owner, row, count)
        shared = which - 2
        return pltpu.make_async_remote_copy(
            src_ref=block, dst_ref=block,
            send_sem=fwd_send.at[shared, peer - 1, step - 1, way],
            recv_sem=fwd_recv.at[shared, peer - 1, step - 1, way],
            device_id={"rep": turn(my_rep, peer, reps)}, device_id_type=MESH)

    def begin(which):
        for way in (0, 1):
            ring(which, 1, way).start()

    def advance(which, step):
        for way in (0, 1):
            ring(which, step, way).wait_recv()
            if step < half:
                ring(which, step + 1, way).start()
            if KINDS[which][2]:
                for peer in range(1, reps):
                    forward(which, step, way, peer).start()

    def tp_copy(stage, offset, source, target):
        return pltpu.make_async_remote_copy(
            src_ref=source, dst_ref=target,
            send_sem=tp_send.at[stage, offset - 1], recv_sem=tp_recv.at[stage, offset - 1],
            device_id={"tp": turn(my_tp, offset, tp)}, device_id_type=MESH)

    def feature_cols(owner):
        return pl.ds(pl.multiple_of(owner * width, 128), width)

    barrier = pltpu.get_barrier_semaphore()
    greeted = 0
    for name, at, count, offsets in (
            ("fs", me, fs, (1, -1)),
            ("tp", my_tp, tp, range(1, tp)),
            ("rep", my_rep, reps, range(1, reps))):
        for offset in offsets:
            pl.semaphore_signal(barrier, inc=1, device_id={name: turn(at, offset, count)},
                                device_id_type=MESH)
            greeted += 1
    pl.semaphore_wait(barrier, greeted)

    begin(0)
    begin(1)
    stream_sends = []
    for offset in range(1, tp):
        copy = tp_copy(0, offset, stream, rows_all.at[:, feature_cols(my_tp)])
        copy.start()
        stream_sends.append(copy)
    keeps = []
    for which in range(len(own)):
        keep = pltpu.make_async_copy(
            own[which], piece(which, me, 0, own[which].shape[0]), own_sem.at[which])
        keep.start()
        keeps.append(keep)
    keep_stream = pltpu.make_async_copy(
        stream, rows_all.at[:, feature_cols(my_tp)], keep_sem)
    keep_stream.start()
    for step in range(1, half):
        advance(0, step)
        advance(1, step)
    begin(2)
    begin(3)

    def norm_into(source, gain, target):
        tile = 64

        def body(i, carry):
            at = pl.ds(pl.multiple_of(i * tile, tile), tile)
            wide = source[at, :].astype(jnp.float32)
            mean = jnp.mean(wide * wide, axis=-1, keepdims=True)
            target[at, :] = (wide * lax.rsqrt(mean + EPSILON)
                             * gain[...].astype(jnp.float32)).astype(jnp.bfloat16)
            return carry

        lax.fori_loop(0, tokens // tile, body, 0)

    keep_stream.wait()
    for copy in stream_sends:
        copy.wait()
    norm_into(rows_all, mix_gain, normed)
    keeps[0].wait()
    advance(0, half)

    local_groups, group_dim = pool_w.shape[0], pool_w.shape[1]
    at_row = lax.broadcasted_iota(jnp.int32, (SEQ, SEQ), 0)
    at_col = lax.broadcasted_iota(jnp.int32, (SEQ, SEQ), 1)
    insides, inverses = [], []
    for g in range(local_groups):
        group = my_tp * local_groups + g
        level = lax.div(4 * group, local_groups * tp)
        reach = jnp.int32(2)
        for bit in range(1, 4):
            reach = jnp.where(level >= bit, jnp.int32(2 << bit), reach)
        inside = (at_col <= at_row) & (at_col > at_row - reach)
        insides.append(jnp.where(inside, 1.0, 0.0).astype(jnp.bfloat16))
        inverses.append(jnp.minimum(at_row + 1, reach).astype(jnp.float32)[:, :1])

    def mix(i, carry):
        at = pl.ds(pl.multiple_of(i * SEQ, SEQ), SEQ)
        pooled = jnp.dot(normed[at, :], in_all[...],
                         preferred_element_type=jnp.float32).astype(jnp.bfloat16)
        for g in range(local_groups):
            cols = slice(g * group_dim, (g + 1) * group_dim)
            part = pooled[:, cols]
            sums = jnp.dot(insides[g], part, preferred_element_type=jnp.float32)
            contrast = (sums / inverses[g] - part.astype(jnp.float32)).astype(jnp.bfloat16)
            mixed = jnp.dot(contrast, pool_w[g], preferred_element_type=jnp.float32)
            group_out[at, cols] = (mixed * scale[:, cols].astype(jnp.float32)).astype(jnp.bfloat16)
        return carry

    lax.fori_loop(0, tokens // SEQ, mix, 0)

    keeps[1].wait()
    advance(1, half)

    def spread(operand, weights, stage, sends, tile):
        def block(owner, target):
            def body(i, carry):
                at = pl.ds(pl.multiple_of(i * tile, tile), tile)
                target[at, :] = jnp.dot(operand[at, :], weights[:, feature_cols(owner)],
                                        preferred_element_type=jnp.float32).astype(jnp.bfloat16)
                return carry
            lax.fori_loop(0, tokens // tile, body, 0)

        copies = []
        recv = mix_recv if stage == 1 else ffn_recv
        for offset in sorted(range(1, tp), key=lambda o: -min(o, tp - o)):
            block(turn(my_tp, offset, tp), sends.at[offset - 1])
            copy = tp_copy(stage, offset, sends.at[offset - 1], recv.at[offset - 1])
            copy.start()
            copies.append(copy)
        block(my_tp, sends.at[tp - 1])
        return copies

    def gather_sum(base, recv, sends, target):
        tile = 64

        def body(i, carry):
            at = pl.ds(pl.multiple_of(i * tile, tile), tile)
            total = sends[tp - 1, at, :].astype(jnp.float32)
            for k in range(tp - 1):
                total = total + recv[k, at, :].astype(jnp.float32)
            target[at, :] = (base[at, :].astype(jnp.float32) + total).astype(jnp.bfloat16)
            return carry

        lax.fori_loop(0, tokens // tile, body, 0)

    mix_copies = spread(group_out, out_all, 1, mix_send, tokens // 2)
    for step in range(1, half):
        advance(2, step)
        advance(3, step)
    begin(4)
    for copy in mix_copies:
        copy.wait()
    gather_sum(stream, mix_recv, mix_send, middle)
    keep_middle = pltpu.make_async_copy(middle, mid_all.at[:, feature_cols(my_tp)], keep_sem)
    keep_middle.start()
    middle_copies = []
    for offset in range(1, tp):
        copy = tp_copy(2, offset, middle, mid_all.at[:, feature_cols(my_tp)])
        copy.start()
        middle_copies.append(copy)
    advance(2, half)
    advance(3, half)
    keep_middle.wait()
    for copy in middle_copies:
        copy.wait()
    norm_into(mid_all, ffn_gain, normed)
    for step in range(1, half + 1):
        advance(4, step)

    def arrived(which):
        keeps[which].wait()
        if KINDS[which][2]:
            for step in range(1, half + 1):
                for way in (0, 1):
                    for peer in range(1, reps):
                        forward(which, step, way, peer).wait()

    arrived(4)
    arrived(2)
    tile = tokens // 2

    def gated(i, carry):
        at = pl.ds(pl.multiple_of(i * tile, tile), tile)
        values = normed[at, :]
        gate = jnp.dot(values, gate_all[...], preferred_element_type=jnp.float32)
        up = jnp.dot(values, up_all[...], preferred_element_type=jnp.float32)
        hidden[at, :] = (gate / (1.0 + jnp.exp(-gate)) * up).astype(jnp.bfloat16)
        return carry

    lax.fori_loop(0, tokens // tile, gated, 0)
    arrived(3)
    ffn_copies = spread(hidden, down_all, 3, ffn_send, tokens // 2)
    for which in range(len(own)):
        for step in range(1, half + 1):
            for way in (0, 1):
                ring(which, step, way).wait_send()
    for copy in ffn_copies:
        copy.wait()
    gather_sum(middle, ffn_recv, ffn_send, result)


def on_device(sizes, stream, in_weight, pool_weight, pool_scale, out_weight,
              mix_gain, ffn_gain, gate_weight, up_weight, down_weight):
    reps, fs, tp = sizes
    half = fs // 2
    tokens, width = stream.shape
    features = width * tp
    own = (in_weight, out_weight, up_weight, down_weight, gate_weight)
    full = [pltpu.VMEM((w.shape[0] * fs, w.shape[1]) if kind[1] else (w.shape[0], w.shape[1] * fs),
                       jnp.bfloat16) for w, kind in zip(own, KINDS)]
    units = gate_weight.shape[1]
    bf = jnp.bfloat16
    vmem = pl.BlockSpec(memory_space=pltpu.VMEM)
    hbm = pl.BlockSpec(memory_space=pl.ANY)
    dma = pltpu.SemaphoreType.DMA
    flops = 2 * tokens * (2 * features * in_weight.shape[1] + 3 * features * units)
    return pl.pallas_call(
        functools.partial(kernel, sizes),
        out_shape=jax.ShapeDtypeStruct(stream.shape, bf),
        in_specs=[vmem] + [hbm] * 5 + [vmem] * 4,
        out_specs=vmem,
        scratch_shapes=full + [
            pltpu.VMEM((tokens, features), bf),
            pltpu.VMEM((tokens, features), bf),
            pltpu.VMEM((tokens, in_weight.shape[1]), bf),
            pltpu.VMEM((tokens, units), bf),
            pltpu.VMEM((tokens, width), bf),
            pltpu.VMEM((tokens, features), bf),
            pltpu.VMEM((tp, tokens, width), bf),
            pltpu.VMEM((tp - 1, tokens, width), bf),
            pltpu.VMEM((tp, tokens, width), bf),
            pltpu.VMEM((tp - 1, tokens, width), bf),
            dma((len(own), half, 2)),
            dma((len(own), half, 2)),
            dma((2, max(reps - 1, 1), half, 2)),
            dma((2, max(reps - 1, 1), half, 2)),
            dma((len(own),)),
            dma((4, tp - 1)),
            dma((4, tp - 1)),
            dma(()),
        ],
        compiler_params=pltpu.CompilerParams(
            collective_id=0, has_side_effects=True, vmem_limit_bytes=64 * 1024 * 1024 - 65536),
        cost_estimate=pl.CostEstimate(flops=flops, bytes_accessed=flops // 512, transcendentals=0),
    )(stream, in_weight, out_weight, up_weight, down_weight, gate_weight, pool_weight,
      pool_scale.reshape(1, -1), mix_gain.reshape(1, -1), ffn_gain.reshape(1, -1))


def solution(mesh):
    sizes = tuple(mesh.shape[name] for name in ("rep", "fs", "tp"))
    return jax.shard_map(
        functools.partial(on_device, sizes),
        mesh=mesh,
        in_specs=(
            P(("rep", "fs"), "tp"),
            P("fs", "tp"),
            P("tp", None, None),
            P("tp"),
            P("tp", "fs"),
            P(),
            P(),
            P("fs", "tp"),
            P("fs", "tp"),
            P("tp", "fs"),
        ),
        out_specs=P(("rep", "fs"), "tp"),
        check_vma=False,
    )
```

```python
import functools

import jax
import jax.numpy as jnp
from jax import lax
from jax.experimental import pallas as pl
from jax.experimental.pallas import tpu as pltpu
from jax.sharding import PartitionSpec as P

SEQ = 128
EPSILON = 1e-06
MESH = pl.DeviceIdType.MESH
BY_ROWS = (True, False, True, True, False)
PIECES = ((0, 0), (1, 0), (2, 0), (3, 0), (2, 1), (3, 1), (4, 0), (4, 1))
CHUNKS = (1, 1, 2, 2, 2)


def kernel(sizes, stream, in_w, out_w, up_w, gate_w, down_w, pool_w, scale,
           mix_gain, ffn_gain, result,
           in_all, out_all, up_all, gate_all, down_all,
           rows_all, normed, group_out, hidden, middle, mid_all,
           mix_send, mix_recv, ffn_send, ffn_recv,
           ring_send, ring_recv, fwd_send, fwd_recv, own_sem,
           tp_send, tp_recv, keep_sem):
    reps, fs, tp = sizes
    half = fs // 2
    my_rep, me, my_tp = lax.axis_index("rep"), lax.axis_index("fs"), lax.axis_index("tp")
    own = (in_w, out_w, up_w, gate_w, down_w)
    full = (in_all, out_all, up_all, gate_all, down_all)
    tokens, width = stream.shape

    def turn(at, by, count):
        return lax.rem(at + by + count, count)

    def piece(which, owner, row, count):
        block_rows, block_cols = own[which].shape
        if BY_ROWS[which]:
            return full[which].at[pl.ds(pl.multiple_of(owner * block_rows + row, 16), count), :]
        return full[which].at[pl.ds(pl.multiple_of(row, 16), count),
                              pl.ds(pl.multiple_of(owner * block_cols, 128), block_cols)]

    def span(number, step, way):
        which, chunk = PIECES[number]
        rows = own[which].shape[0]
        cut = rows % (CHUNKS[which] * reps * 2 * 16) == 0
        count = rows // CHUNKS[which] if cut else (rows, 0)[chunk]
        row = chunk * (rows // CHUNKS[which])
        count = count // reps
        row = row + my_rep * count
        if step == half:
            count = count // 2
            row = row + way * count
        return which, row, count

    def empty(number):
        return span(number, 1, 0)[2] == 0

    def ring(number, step, way):
        which, row, count = span(number, step, way)
        sign = 1 - 2 * way
        owner = turn(me, -sign * (step - 1), fs)
        if step == 1:
            source = own[which].at[pl.ds(pl.multiple_of(row, 16), count), :]
        else:
            source = piece(which, owner, row, count)
        return pltpu.make_async_remote_copy(
            src_ref=source, dst_ref=piece(which, owner, row, count),
            send_sem=ring_send.at[number, step - 1, way],
            recv_sem=ring_recv.at[number, step - 1, way],
            device_id={"fs": turn(me, sign, fs)}, device_id_type=MESH)

    def forward(number, step, way, peer):
        which, row, count = span(number, step, way)
        block = piece(which, turn(me, -(1 - 2 * way) * step, fs), row, count)
        return pltpu.make_async_remote_copy(
            src_ref=block, dst_ref=block,
            send_sem=fwd_send.at[number, peer - 1, step - 1, way],
            recv_sem=fwd_recv.at[number, peer - 1, step - 1, way],
            device_id={"rep": turn(my_rep, peer, reps)}, device_id_type=MESH)

    def begin(*numbers):
        for number in numbers:
            if not empty(number):
                for way in (0, 1):
                    ring(number, 1, way).start()

    def advance(number, step):
        if empty(number):
            return
        for way in (0, 1):
            ring(number, step, way).wait_recv()
            if step < half:
                ring(number, step + 1, way).start()
            for peer in range(1, reps):
                forward(number, step, way, peer).start()

    def early(*numbers):
        for number in numbers:
            for step in range(1, half):
                advance(number, step)

    def late(*numbers):
        for number in numbers:
            advance(number, half)

    def arrived(*numbers):
        for number in numbers:
            if PIECES[number][1] == 0:
                keeps[PIECES[number][0]].wait()
            if empty(number):
                continue
            for step in range(1, half + 1):
                for way in (0, 1):
                    for peer in range(1, reps):
                        forward(number, step, way, peer).wait()

    def tp_copy(stage, offset, source, target):
        return pltpu.make_async_remote_copy(
            src_ref=source, dst_ref=target,
            send_sem=tp_send.at[stage, offset - 1], recv_sem=tp_recv.at[stage, offset - 1],
            device_id={"tp": turn(my_tp, offset, tp)}, device_id_type=MESH)

    def feature_cols(owner):
        return pl.ds(pl.multiple_of(owner * width, 128), width)

    barrier = pltpu.get_barrier_semaphore()
    greeted = 0
    for name, at, count, offsets in (
            ("fs", me, fs, (1, -1)),
            ("tp", my_tp, tp, range(1, tp)),
            ("rep", my_rep, reps, range(1, reps))):
        for offset in offsets:
            pl.semaphore_signal(barrier, inc=1, device_id={name: turn(at, offset, count)},
                                device_id_type=MESH)
            greeted += 1
    pl.semaphore_wait(barrier, greeted)

    begin(0, 1)
    stream_sends = []
    for offset in range(1, tp):
        copy = tp_copy(0, offset, stream, rows_all.at[:, feature_cols(my_tp)])
        copy.start()
        stream_sends.append(copy)
    keeps = []
    for which in range(len(own)):
        keep = pltpu.make_async_copy(
            own[which], piece(which, me, 0, own[which].shape[0]), own_sem.at[which])
        keep.start()
        keeps.append(keep)
    keep_stream = pltpu.make_async_copy(
        stream, rows_all.at[:, feature_cols(my_tp)], keep_sem)
    keep_stream.start()
    early(0, 1)
    begin(2, 3, 4)
    late(0, 1)

    def norm_into(source, gain, target):
        tile = 64

        def body(i, carry):
            at = pl.ds(pl.multiple_of(i * tile, tile), tile)
            wide = source[at, :].astype(jnp.float32)
            mean = jnp.mean(wide * wide, axis=-1, keepdims=True)
            target[at, :] = (wide * lax.rsqrt(mean + EPSILON)
                             * gain[...].astype(jnp.float32)).astype(jnp.bfloat16)
            return carry

        lax.fori_loop(0, tokens // tile, body, 0)

    keep_stream.wait()
    for copy in stream_sends:
        copy.wait()
    norm_into(rows_all, mix_gain, normed)
    arrived(0)

    local_groups, group_dim = pool_w.shape[0], pool_w.shape[1]
    at_row = lax.broadcasted_iota(jnp.int32, (SEQ, SEQ), 0)
    at_col = lax.broadcasted_iota(jnp.int32, (SEQ, SEQ), 1)
    insides, inverses = [], []
    for g in range(local_groups):
        group = my_tp * local_groups + g
        level = lax.div(4 * group, local_groups * tp)
        reach = jnp.int32(2)
        for bit in range(1, 4):
            reach = jnp.where(level >= bit, jnp.int32(2 << bit), reach)
        inside = (at_col <= at_row) & (at_col > at_row - reach)
        insides.append(jnp.where(inside, 1.0, 0.0).astype(jnp.bfloat16))
        inverses.append(jnp.minimum(at_row + 1, reach).astype(jnp.float32)[:, :1])

    def mix(i, carry):
        at = pl.ds(pl.multiple_of(i * SEQ, SEQ), SEQ)
        pooled = jnp.dot(normed[at, :], in_all[...],
                         preferred_element_type=jnp.float32).astype(jnp.bfloat16)
        for g in range(local_groups):
            cols = slice(g * group_dim, (g + 1) * group_dim)
            part = pooled[:, cols]
            sums = jnp.dot(insides[g], part, preferred_element_type=jnp.float32)
            contrast = (sums / inverses[g] - part.astype(jnp.float32)).astype(jnp.bfloat16)
            mixed = jnp.dot(contrast, pool_w[g], preferred_element_type=jnp.float32)
            group_out[at, cols] = (mixed * scale[:, cols].astype(jnp.float32)).astype(jnp.bfloat16)
        return carry

    lax.fori_loop(0, tokens // SEQ, mix, 0)

    arrived(1)
    early(2)

    def spread(operand, weights, stage, sends, tile):
        def block(owner, target):
            def body(i, carry):
                at = pl.ds(pl.multiple_of(i * tile, tile), tile)
                target[at, :] = jnp.dot(operand[at, :], weights[:, feature_cols(owner)],
                                        preferred_element_type=jnp.float32).astype(jnp.bfloat16)
                return carry
            lax.fori_loop(0, tokens // tile, body, 0)

        copies = []
        recv = mix_recv if stage == 1 else ffn_recv
        for offset in sorted(range(1, tp), key=lambda o: -min(o, tp - o)):
            block(turn(my_tp, offset, tp), sends.at[offset - 1])
            copy = tp_copy(stage, offset, sends.at[offset - 1], recv.at[offset - 1])
            copy.start()
            copies.append(copy)
        block(my_tp, sends.at[tp - 1])
        return copies

    def gather_sum(base, recv, sends, target):
        tile = 64

        def body(i, carry):
            at = pl.ds(pl.multiple_of(i * tile, tile), tile)
            total = sends[tp - 1, at, :].astype(jnp.float32)
            for k in range(tp - 1):
                total = total + recv[k, at, :].astype(jnp.float32)
            target[at, :] = (base[at, :].astype(jnp.float32) + total).astype(jnp.bfloat16)
            return carry

        lax.fori_loop(0, tokens // tile, body, 0)

    mix_copies = spread(group_out, out_all, 1, mix_send, tokens // 2)
    early(3)
    begin(5)
    for copy in mix_copies:
        copy.wait()
    gather_sum(stream, mix_recv, mix_send, middle)
    keep_middle = pltpu.make_async_copy(middle, mid_all.at[:, feature_cols(my_tp)], keep_sem)
    keep_middle.start()
    middle_copies = []
    for offset in range(1, tp):
        copy = tp_copy(2, offset, middle, mid_all.at[:, feature_cols(my_tp)])
        copy.start()
        middle_copies.append(copy)
    early(4)
    begin(6, 7)
    late(2, 3)
    keep_middle.wait()
    for copy in middle_copies:
        copy.wait()
    norm_into(mid_all, ffn_gain, normed)
    early(5)
    late(4)
    early(6)
    late(5)
    early(7)
    late(6)
    arrived(2, 3, 4, 5)
    tile = tokens // 2

    def gated(i, carry):
        at = pl.ds(pl.multiple_of(i * tile, tile), tile)
        values = normed[at, :]
        gate = jnp.dot(values, gate_all[...], preferred_element_type=jnp.float32)
        up = jnp.dot(values, up_all[...], preferred_element_type=jnp.float32)
        hidden[at, :] = (gate / (1.0 + jnp.exp(-gate)) * up).astype(jnp.bfloat16)
        return carry

    lax.fori_loop(0, tokens // tile, gated, 0)
    late(7)
    arrived(6, 7)
    ffn_copies = spread(hidden, down_all, 3, ffn_send, tokens // 2)
    for number in range(len(PIECES)):
        if not empty(number):
            for step in range(1, half + 1):
                for way in (0, 1):
                    ring(number, step, way).wait_send()
    for copy in ffn_copies:
        copy.wait()
    gather_sum(middle, ffn_recv, ffn_send, result)


def on_device(sizes, stream, in_weight, pool_weight, pool_scale, out_weight,
              mix_gain, ffn_gain, gate_weight, up_weight, down_weight):
    reps, fs, tp = sizes
    half = fs // 2
    tokens, width = stream.shape
    features = width * tp
    own = (in_weight, out_weight, up_weight, gate_weight, down_weight)
    full = [pltpu.VMEM((w.shape[0] * fs, w.shape[1]) if by_rows else (w.shape[0], w.shape[1] * fs),
                       jnp.bfloat16) for w, by_rows in zip(own, BY_ROWS)]
    units = gate_weight.shape[1]
    bf = jnp.bfloat16
    vmem = pl.BlockSpec(memory_space=pltpu.VMEM)
    hbm = pl.BlockSpec(memory_space=pl.ANY)
    dma = pltpu.SemaphoreType.DMA
    flops = 2 * tokens * (2 * features * in_weight.shape[1] + 3 * features * units)
    return pl.pallas_call(
        functools.partial(kernel, sizes),
        out_shape=jax.ShapeDtypeStruct(stream.shape, bf),
        in_specs=[vmem] + [hbm] * 5 + [vmem] * 4,
        out_specs=vmem,
        scratch_shapes=full + [
            pltpu.VMEM((tokens, features), bf),
            pltpu.VMEM((tokens, features), bf),
            pltpu.VMEM((tokens, in_weight.shape[1]), bf),
            pltpu.VMEM((tokens, units), bf),
            pltpu.VMEM((tokens, width), bf),
            pltpu.VMEM((tokens, features), bf),
            pltpu.VMEM((tp, tokens, width), bf),
            pltpu.VMEM((tp - 1, tokens, width), bf),
            pltpu.VMEM((tp, tokens, width), bf),
            pltpu.VMEM((tp - 1, tokens, width), bf),
            dma((len(PIECES), half, 2)),
            dma((len(PIECES), half, 2)),
            dma((len(PIECES), max(reps - 1, 1), half, 2)),
            dma((len(PIECES), max(reps - 1, 1), half, 2)),
            dma((len(own),)),
            dma((4, tp - 1)),
            dma((4, tp - 1)),
            dma(()),
        ],
        compiler_params=pltpu.CompilerParams(
            collective_id=0, has_side_effects=True, vmem_limit_bytes=64 * 1024 * 1024 - 65536),
        cost_estimate=pl.CostEstimate(flops=flops, bytes_accessed=flops // 512, transcendentals=0),
    )(stream, in_weight, out_weight, up_weight, gate_weight, down_weight, pool_weight,
      pool_scale.reshape(1, -1), mix_gain.reshape(1, -1), ffn_gain.reshape(1, -1))


def solution(mesh):
    sizes = tuple(mesh.shape[name] for name in ("rep", "fs", "tp"))
    return jax.shard_map(
        functools.partial(on_device, sizes),
        mesh=mesh,
        in_specs=(
            P(("rep", "fs"), "tp"),
            P("fs", "tp"),
            P("tp", None, None),
            P("tp"),
            P("tp", "fs"),
            P(),
            P(),
            P("fs", "tp"),
            P("fs", "tp"),
            P("tp", "fs"),
        ),
        out_specs=P(("rep", "fs"), "tp"),
        check_vma=False,
    )
```
